128 devices in a mesh: sp: 64 (over z, y, x), tp: 2 (over core).
Axes of the slice: x: 4, y: 4, z: 4, core: 2. Of those that a mesh axis runs over, the one named last changes fastest.
Arguments:
- residual: bfloat16 [16384, 2048], P(('sp', 'tp')), may hold values from -6 to 6
- query_rows: bfloat16 [16384, 1024], P('sp', 'tp'), may hold values from -141 to 141
- key_rows: bfloat16 [16384, 1024], P('sp', 'tp'), may hold values from -7.8 to 7.8
- value_rows: bfloat16 [16384, 1024], P('sp', 'tp'), may hold values from -6 to 6
- mix_lambda: float32 [8], P('tp'), may hold values from 0.3 to 0.8
- documents: int32 [16384], P('sp'), may hold values from 0 to 31, never falling along the last dimension, each value on 1 to 768 neighbouring positions
- out_weight: bfloat16 [1024, 2048], replicated, may hold values from -0.1875 to 0.1875
- norm_gain: float32 [2048], replicated, may hold values from 0.1 to 1.9
- gate_weight: bfloat16 [64, 2048, 2048], P('sp', None, 'tp'), may hold values from -0.125 to 0.125
- up_weight: bfloat16 [64, 2048, 2048], P('sp', None, 'tp'), may hold values from -0.125 to 0.125
- down_weight: bfloat16 [64, 2048, 2048], P('sp', 'tp'), may hold values from -0.125 to 0.125
- routes: int32 [16384, 2], P(('sp', 'tp')), may hold values from 0 to 63, all different within a row; in each aligned block of 128 rows (0 to 127, 128 to 255, ...) at most 8 rows name the same one
- route_weights: float32 [16384, 2], P(('sp', 'tp')), may hold values from 0.25 to 1
Outputs:
- layer_out: bfloat16 [16384, 2048], P(('sp', 'tp'))
The draws below stay inside these ranges and needn't reach their ends.
Inputs may be any that keep to these rules, and one draw needn't show every extreme that they name: `documents`: document numbers never fall along the sequence; a document covers at most 768 positions, and one covers exactly that many. `routes`: each row names two different experts. Among the rows of one index of sp+tp, no expert is named by more than 8 rows, and in every draw some expert is named by exactly 8 rows of some such block.
All inputs are finite; a program needn't handle non-finite values.
Results may differ from the reference program's by a relative error of at most 0.013.
Values may be sent and summed in bfloat16 or wider, within the bound.
A program may use at most 128 MiB of HBM per device.

```python
import math
import jax
import jax.numpy as jnp
import numpy as np
from jax import lax

D = 2048
HEADS = 8
HD = 64
VD = 128
FFE = 2048
TOK_DEV = 256
REACH = 3
TOKENS = 16384
EXPERTS = 64
CAP = 8
DOCS = 32
N_SP = 64
N_TP = 2


def drawn_pair(key):
    shape_rows = (TOKENS, HEADS * 2 * HD)
    base_query = jnp.clip(1.3 * jax.random.normal(jax.random.fold_in(key, 101), shape_rows, jnp.float32), -7.8, 7.8)
    base_keys = jnp.clip(1.3 * jax.random.normal(jax.random.fold_in(key, 102), shape_rows, jnp.float32), -7.8, 7.8)
    return (base_query, base_keys)


def draw_query_rows(key, part):
    return drawn_pair(key)[0].astype(jnp.bfloat16)


def draw_key_rows(key, part):
    return drawn_pair(key)[1].astype(jnp.bfloat16)


def steps_of(rng, dims, pieces, low, high):
    factor_of, own = 1.0, jax.random.fold_in(rng, 6)
    for axis_at, parts in pieces:
        steps = jnp.exp(jax.random.uniform(jax.random.fold_in(own, axis_at), (parts,), jnp.float32, low / len(pieces), high / len(pieces)))
        factor_of = factor_of * jnp.repeat(steps, dims[axis_at] // parts).reshape([-1 if axis == axis_at else 1 for axis in range(len(dims))])
    return factor_of


def split_up(count, total, most, slope):
    loads = [(1 << 20) // math.isqrt(rank ** slope) + 1 for rank in range(2, count + 1)]
    rest, counts = total - most - (count - 1), [1] * (count - 1)
    while rest > 0:
        candidates = [i for i in range(count - 1) if counts[i] < most]
        pool, remaining = sum([loads[i] for i in candidates]), rest
        for i in candidates:
            addition = min(most - counts[i], max(1, remaining * loads[i] // pool), rest)
            counts[i] = counts[i] + addition
            rest = rest - addition
    return np.array([most] + counts)


def uneven_parts(rng, amount, total, limit, lean):
    if amount == 2:
        one = jax.random.randint(rng, (), max(1, total - limit), min(limit, total - 1) + 1)
        return jnp.stack([one, total - one])
    lengths = jnp.asarray(split_up(amount, total, limit, lean), jnp.int32)
    pairs = (amount - 1) // 2
    donor, receiver = lengths[1:1 + 2 * pairs:2], lengths[2:2 + 2 * pairs:2]
    slack = jnp.minimum(donor - 1, limit - receiver)
    shifted = jax.random.randint(jax.random.fold_in(rng, 1), (pairs,), 0, 1 << 20) % (slack + 1)
    lengths = lengths.at[1:1 + 2 * pairs:2].set(donor - shifted).at[2:2 + 2 * pairs:2].set(receiver + shifted)
    return lengths[jax.random.permutation(jax.random.fold_in(rng, 2), amount)]


def assign_block(own_key, own, number, rows, count, top, reach, lean):
    ranking = jax.random.permutation(own_key, count)
    crowded, usual = portions_of(count, rows * top, reach, lean, True), portions_of(count, rows * top, reach, lean, False)
    places = jnp.arange(count)

    def named(sizes, offset_by):
        used = int((sizes > 0).sum())
        fixed = max(1, used // 4)
        passed = fixed + (places - fixed + offset_by * (used - fixed)) % max(1, count - fixed)
        return jnp.zeros((count,), jnp.int32).at[ranking[jnp.where(places < fixed, places, passed)]].set(jnp.asarray(sizes, jnp.int32))

    sizes = jnp.where(number % 4 == 0, named(crowded, number // 4), named(usual, number - number // 4 - 1))
    mixed = jax.random.permutation(jax.random.fold_in(own, 3), count)
    donor, sink = mixed[0:count // 2 * 2:2], mixed[1:count // 2 * 2:2]
    slack = jnp.minimum(sizes[donor] - 1, reach - sizes[sink]) // 2
    slack = jnp.where((donor == ranking[0]) | (sink == ranking[0]) | (sizes[sink] == 0), 0, jnp.maximum(slack, 0))
    passed = jax.random.randint(jax.random.fold_in(own, 4), (count // 2,), 0, 1 << 20) % (slack + 1)
    sizes = sizes.at[donor].add(-passed).at[sink].add(passed)
    items = jnp.searchsorted(jnp.cumsum(sizes), jnp.arange(rows * top), side="right").astype(jnp.int32)
    table = items.reshape(top, rows).T
    table = table[jax.random.permutation(jax.random.fold_in(own, 1), rows)]
    offset_by = jax.random.randint(jax.random.fold_in(own, 2), (rows, 1), 0, top)
    return jnp.take_along_axis(table, (jnp.arange(top)[None, :] + offset_by) % top, axis=1)


def portions_of(amount, total, reach, slope, full):
    weights = [(1 << 20) // math.isqrt(grade ** slope) + 1 for grade in range(1, amount + 1)]
    largest = reach if full else min(reach, max(-(-total // amount), total * weights[0] // sum(weights)))
    least = 1 if total - largest >= amount - 1 else 0
    holding, rest = [largest] + [least] * (amount - 1), total - largest - least * (amount - 1)
    while rest > 0:
        candidates = [i for i in range(1, amount) if holding[i] < largest] or [i for i in range(1, amount) if holding[i] < reach]
        pool, budget = sum([weights[i] for i in candidates]), rest
        for i in candidates:
            more = min(reach - holding[i], max(1, budget * weights[i] // pool), rest)
            holding[i] = holding[i] + more
            rest = rest - more
    return np.array(holding)


def normal_values(own_key, shape, deviation, limit, cuts=(), held_as=jnp.bfloat16):
    level = steps_of(own_key, shape, cuts, -0.22, 0.18) if cuts else 1.0
    values = jax.random.normal(own_key, shape, jnp.float32) * deviation * level
    return jnp.minimum(jnp.maximum(values, -limit), limit).astype(held_as)


def setup_inputs(seed: int = 0) -> dict:
    keys = jax.random.split(jax.random.key(seed), 14)
    residual = normal_values(keys[0], (TOKENS, D), 1.0, 6.0, ((0, 128),))
    query_rows = draw_query_rows(jax.random.fold_in(keys[13], 71), 0)
    key_rows = draw_key_rows(jax.random.fold_in(keys[13], 71), 0)
    value_rows = normal_values(keys[3], (TOKENS, HEADS * VD), 1.0, 6.0, ((0, 64), (1, 2)))
    mix_lambda = jnp.clip(0.3 + 0.5 * jax.random.uniform(keys[4], (HEADS,), jnp.float32) ** steps_of(keys[4], (HEADS,), ((0, 2),), -0.2, 0.2), 0.3, 0.8)
    documents = jnp.searchsorted(jnp.cumsum(uneven_parts(keys[5], DOCS, TOKENS, REACH * TOK_DEV, 0)), jnp.arange(TOKENS), side="right").astype(jnp.int32)
    out_weight = normal_values(keys[6], (HEADS * VD, D), (HEADS * VD) ** -0.5, 0.1875)
    norm_gain = jnp.clip(1.0 + 0.18 * jax.random.normal(keys[7], (D,), jnp.float32), 0.1, 1.9)
    gate_weight = normal_values(keys[8], (EXPERTS, D, FFE), D ** -0.5, 0.125, ((0, 64), (2, 2)))
    up_weight = normal_values(keys[9], (EXPERTS, D, FFE), D ** -0.5, 0.125, ((0, 64), (2, 2)))
    down_weight = normal_values(keys[10], (EXPERTS, FFE, D), FFE ** -0.5, 0.125, ((0, 64), (1, 2)))
    routes_keys = jax.random.split(jax.random.fold_in(keys[11], 1), TOKENS // (TOK_DEV // 2))
    routes_turns = jax.random.permutation(jax.random.fold_in(keys[11], 3), TOKENS // (TOK_DEV // 2))
    routes = jax.vmap(lambda own, number: assign_block(jax.random.fold_in(keys[11], 2), own, number, TOK_DEV // 2, EXPERTS, 2, CAP, 2))(routes_keys, routes_turns).reshape((TOKENS, 2))
    route_weights = jnp.clip(0.25 + 0.75 * jax.random.uniform(keys[12], (TOKENS, 2), jnp.float32) ** steps_of(keys[12], (TOKENS, 2), ((0, 128),), -0.2, 0.2), 0.25, 1.0)
    return {"residual": residual, "query_rows": query_rows, "key_rows": key_rows, "value_rows": value_rows, "mix_lambda": mix_lambda, "documents": documents, "out_weight": out_weight, "norm_gain": norm_gain, "gate_weight": gate_weight, "up_weight": up_weight, "down_weight": down_weight, "routes": routes, "route_weights": route_weights}


def rms_rows(values_in):
    return values_in * lax.rsqrt(lax.optimization_barrier(jnp.mean(values_in * values_in, axis=-1, keepdims=True)) + 1e-06)

def reference(residual, query_rows, key_rows, value_rows, mix_lambda, documents, out_weight, norm_gain, gate_weight, up_weight, down_weight, routes, route_weights):
    score_scale = HD ** (-0.5)
    queries = query_rows.reshape(TOKENS // TOK_DEV, TOK_DEV, HEADS, 2, HD)
    all_keys = key_rows.reshape(TOKENS, HEADS, 2, HD).astype(jnp.float32)
    all_values = value_rows.reshape(TOKENS, HEADS, VD).astype(jnp.float32)
    block_ids = documents.reshape(TOKENS // TOK_DEV, TOK_DEV)

    def attend(operands):
        block_query, query_ids = operands
        scores = jnp.einsum('qhcd,khcd->hcqk', block_query.astype(jnp.float32), all_keys) * score_scale
        same_document = query_ids[:, None] == documents[None, :]
        masked = jnp.where(same_document[None, None], scores, -1e+30)
        largest = lax.optimization_barrier(jnp.max(masked, axis=-1, keepdims=True))
        lifted = jnp.exp(masked - largest)
        probabilities = lifted / lax.optimization_barrier(jnp.sum(lifted, axis=-1, keepdims=True))
        weights = (probabilities[:, 0] - mix_lambda[:, None, None] * probabilities[:, 1]).astype(jnp.bfloat16)
        head_out = jnp.einsum('hqk,khd->qhd', weights.astype(jnp.float32), all_values)
        head_normed = rms_rows(head_out).astype(jnp.bfloat16)
        return head_normed.reshape(TOK_DEV, HEADS * VD)
    head_rows = lax.map(attend, (queries, block_ids)).reshape(TOKENS, HEADS * VD)
    projected = jnp.dot(head_rows, out_weight, preferred_element_type=jnp.float32)
    mixed = (residual.astype(jnp.float32) + projected).astype(jnp.bfloat16)
    normed = (rms_rows(mixed.astype(jnp.float32)) * norm_gain).astype(jnp.bfloat16)
    top_count = routes.shape[1]
    assign_count = TOKENS * top_count
    flat_routes = routes.reshape(-1)
    padded_rows = jnp.concatenate([normed, jnp.zeros((1, D), jnp.bfloat16)], axis=0)
    most_rows = N_SP * N_TP * CAP
    half_width = FFE // N_TP

    def one_expert(collected, expert):
        chosen = jnp.nonzero(flat_routes == expert, size=most_rows, fill_value=assign_count)[0].astype(jnp.int32)
        picked = padded_rows[chosen // top_count]
        gate = jnp.dot(picked, gate_weight[expert], preferred_element_type=jnp.float32)
        upward = jnp.dot(picked, up_weight[expert], preferred_element_type=jnp.float32)
        hidden = (jax.nn.silu(gate) * upward).astype(jnp.bfloat16)
        hidden_halves = hidden.reshape(most_rows, N_TP, half_width).astype(jnp.float32)
        down_halves = down_weight[expert].reshape(N_TP, half_width, D).astype(jnp.float32)
        partial_value = jnp.einsum('rhp,hpd->hrd', hidden_halves, down_halves).astype(jnp.bfloat16)
        expert_out = lax.optimization_barrier(jnp.sum(partial_value.astype(jnp.float32), axis=0)).astype(jnp.bfloat16)
        return (collected.at[chosen].set(expert_out), None)
    collected, _ = lax.scan(one_expert, jnp.zeros((assign_count + 1, D), jnp.bfloat16), jnp.arange(EXPERTS, dtype=jnp.int32))
    outputs = collected[:assign_count].reshape(TOKENS, top_count, D).astype(jnp.float32)
    weighted = lax.optimization_barrier(jnp.sum(outputs * route_weights[:, :, None], axis=1))
    return (mixed.astype(jnp.float32) + weighted).astype(jnp.bfloat16)
```

```python
import functools

import jax
import jax.numpy as jnp
from jax import lax
from jax.experimental import pallas as pl
from jax.experimental.pallas import tpu as pltpu
from jax.sharding import PartitionSpec as P

MESH = pl.DeviceIdType.MESH
VMEM = pl.BlockSpec(memory_space=pltpu.VMEM)
ANY = pl.BlockSpec(memory_space=pl.ANY)

CHIPS = 64
GROUP = 4
GROUPS = CHIPS // GROUP
LEN = 256
TILE = 128
HW = 128
REACH = 3
SLOTS = 2 * REACH + GROUP
WINDOW = 13
CAP = 8
D = 2048
FF = 1024
CHUNKS = 4
PER = CHIPS // CHUNKS
ROWS = PER * CAP
STRIDE = 37
FIRST = 16
ORDER = ((2, 0), (1, 0), (3, 0), (2, 1), (1, 1), (3, 1))
ARRIVE = ((1, 0), (3, 0), (2, 0), (1, 1), (3, 1), (2, 1))
TAIL = 48
GATE = (4, 4, 4, 4)
EARLY = 7


def remote(src, dst, send, recv, sp, tp):
    return pltpu.make_async_remote_copy(
        src_ref=src,
        dst_ref=dst,
        send_sem=send,
        recv_sem=recv,
        device_id=(sp, tp),
        device_id_type=MESH,
    )


def gather_kernel(
    q_hbm,
    k_hbm,
    v_hbm,
    doc_hbm,
    lam_hbm,
    qg,
    kg,
    vg,
    ig,
    lg,
    q_ref,
    k_ref,
    v_ref,
    doc_ref,
    lam_ref,
    own_ids,
    lsem,
    xsend,
    xrecv,
    ysend,
    yrecv,
):
    me, core = lax.axis_index("sp"), lax.axis_index("tp")
    x, group = me % GROUP, me // GROUP
    up = ((group + 1) % GROUPS) * GROUP + x
    down = ((group + GROUPS - 1) % GROUPS) * GROUP + x
    base = group * GROUP
    barrier = pltpu.get_barrier_semaphore()
    for step in (1, 2, 3):
        pl.semaphore_signal(
            barrier, inc=1, device_id=(base + (x + step) % GROUP, core), device_id_type=MESH
        )
    for other in (up, down):
        pl.semaphore_signal(barrier, inc=1, device_id=(other, core), device_id_type=MESH)
    loads = [
        pltpu.make_async_copy(src, dst, lsem.at[i])
        for i, (src, dst) in enumerate(
            (
                (doc_hbm, doc_ref),
                (k_hbm, k_ref),
                (v_hbm, v_ref),
                (q_hbm, q_ref),
                (lam_hbm, lam_ref),
            )
        )
    ]
    for load in loads:
        load.start()
    loads[0].wait()
    loads[4].wait()
    at_x = lax.broadcasted_iota(jnp.int32, (1, GROUP), 1) == x
    lam = jnp.sum(jnp.where(at_x, lam_ref[...], 0.0), axis=1, keepdims=True)
    lg[...] = jnp.broadcast_to(lam, (8, TILE))
    for half in range(2):
        own_ids[half] = jnp.broadcast_to(doc_ref[half : half + 1, :], (8, TILE))
    pl.semaphore_wait(barrier, 5)
    for load in loads[1:4]:
        load.wait()

    def columns(ref, at):
        return ref.at[:, pl.ds(pl.multiple_of(at * HW, HW), HW)]

    def across(step):
        to = (x + step) % GROUP
        pairs = (
            (columns(k_ref, to), kg.at[REACH + x]),
            (columns(v_ref, to), vg.at[REACH + x]),
            (own_ids, ig.at[REACH + x]),
            (columns(q_ref, to), qg.at[x]),
        )
        return [
            remote(src, dst, xsend.at[step - 1, i], xrecv.at[step - 1, i], base + to, core)
            for i, (src, dst) in enumerate(pairs)
        ]

    def along(source, right, i):
        slot = REACH + source
        there = source - 1 if right else REACH + GROUP + source
        way = 0 if right else 1
        at = jnp.clip(source - 1 if right else source, 0, 2)
        ref = (kg, vg, ig)[i]
        return remote(
            ref.at[slot],
            ref.at[there],
            ysend.at[way, at, i],
            yrecv.at[way, at, i],
            up if right else down,
            core,
        )

    def forward(source, *which):
        @pl.when(source >= 1)
        def _():
            for i in which:
                along(source, True, i).start()

        @pl.when(source <= 2)
        def _():
            for i in which:
                along(source, False, i).start()

    sends = {step: across(step) for step in (1, 2, 3)}
    for step, part in ORDER:
        sends[step][part].start()
    for step in (2, 1, 3):
        sends[step][2].start()
        sends[step][3].start()
    mine = pl.ds(pl.multiple_of(x * HW, HW), HW)
    kg[REACH + x] = k_ref[:, mine]
    vg[REACH + x] = v_ref[:, mine]
    ig[REACH + x] = own_ids[...]
    qg[x] = q_ref[:, mine]
    forward(x, 0, 1, 2)
    for step, part in ARRIVE:
        sends[step][part].wait_recv()
        forward((x + GROUP - step) % GROUP, part)
    for step in (1, 3, 2):
        sends[step][2].wait_recv()
        forward((x + GROUP - step) % GROUP, 2)
    for step in (1, 2, 3):
        sends[step][3].wait_recv()
        for copy in sends[step]:
            copy.wait_send()
    for source in range(GROUP):
        for i in range(3):
            if source >= 1:
                along(source, True, i).wait()
            if source <= 2:
                along(source, False, i).wait()


def gathered(q, k, v, documents, lam):
    return pl.pallas_call(
        gather_kernel,
        out_shape=(
            pltpu.VMEM((GROUP, LEN, HW), jnp.bfloat16),
            pltpu.VMEM((SLOTS, LEN, HW), jnp.bfloat16),
            pltpu.VMEM((SLOTS, LEN, HW), jnp.bfloat16),
            pltpu.VMEM((SLOTS, 2, 8, TILE), jnp.int32),
            pltpu.VMEM((8, TILE), jnp.float32),
        ),
        in_specs=[ANY] * 5,
        out_specs=(VMEM,) * 5,
        scratch_shapes=[
            pltpu.VMEM((LEN, GROUP * HW), jnp.bfloat16),
            pltpu.VMEM((LEN, GROUP * HW), jnp.bfloat16),
            pltpu.VMEM((LEN, GROUP * HW), jnp.bfloat16),
            pltpu.VMEM((2, TILE), jnp.int32),
            pltpu.VMEM((1, GROUP), jnp.float32),
            pltpu.VMEM((2, 8, TILE), jnp.int32),
            pltpu.SemaphoreType.DMA((5,)),
            pltpu.SemaphoreType.DMA((3, 4)),
            pltpu.SemaphoreType.DMA((3, 4)),
            pltpu.SemaphoreType.DMA((2, 3, 3)),
            pltpu.SemaphoreType.DMA((2, 3, 3)),
        ],
        compiler_params=pltpu.CompilerParams(collective_id=0, has_side_effects=True),
    )(*(pltpu.with_memory_space_constraint(a, pltpu.HBM) for a in (q, k, v, documents.reshape(2, TILE), lam.reshape(1, GROUP))))


def main_kernel(
    q_ref,
    k_ref,
    v_ref,
    id_ref,
    lam_ref,
    route_hbm,
    res_hbm,
    gain_hbm,
    rw_hbm,
    wout_hbm,
    gate_hbm,
    up_hbm,
    down_hbm,
    out_ref,
    route_ref,
    res_ref,
    gain_ref,
    rw_ref,
    wout,
    gate,
    upw,
    down,
    hsend,
    heads,
    mixed,
    outgoing,
    rows,
    hidden,
    part,
    theirs,
    answer,
    returned,
    pick,
    normed,
    sums,
    wsem,
    hs,
    hr,
    ds_,
    dr,
    fs,
    fr,
    ps,
    pr,
    rs,
    rr,
):
    me, core = lax.axis_index("sp"), lax.axis_index("tp")
    x, base = me % GROUP, (me // GROUP) * GROUP
    other = 1 - core
    barrier = pltpu.get_barrier_semaphore()

    mx, my, mz = lax.rem(me, 4), lax.rem(lax.div(me, 4), 4), lax.div(me, 16)

    def place(i, sign):
        mix = lax.rem(i * STRIDE, CHIPS)
        px = lax.rem(mx + sign * mix + CHIPS, 4)
        py = lax.rem(my + sign * lax.div(mix, 4) + CHIPS, 4)
        pz = lax.rem(mz + sign * lax.div(mix, 16) + CHIPS, 4)
        return pz * 16 + py * 4 + px

    def greet(i, _):
        pl.semaphore_signal(barrier, inc=1, device_id=(lax.rem(me + i, CHIPS), core), device_id_type=MESH)
        return 0

    lax.fori_loop(1, CHIPS, greet, 0)
    for step in range(GROUP):
        pl.semaphore_signal(
            barrier, inc=1, device_id=(base + (x + step) % GROUP, other), device_id_type=MESH
        )
    loads = [
        pltpu.make_async_copy(src, dst, wsem.at[i])
        for i, (src, dst) in enumerate(
            (
                (route_hbm, route_ref),
                (res_hbm, res_ref),
                (gain_hbm, gain_ref),
                (rw_hbm, rw_ref),
                (wout_hbm, wout),
                (gate_hbm.at[0], gate),
                (up_hbm.at[0], upw),
                (down_hbm.at[0], down),
            )
        )
    ]
    for load in loads:
        load.start()

    def column(row):
        return jnp.transpose(jnp.broadcast_to(row.astype(jnp.float32), (TILE, TILE)))

    def wide(row):
        return jnp.concatenate([column(row)] * 4, axis=1)

    lam = lam_ref[0:1, 0:1]
    my_head = core * GROUP + x
    mine = 2 * x + core
    my_columns = pl.ds(pl.multiple_of(my_head * HW, HW), HW)
    low = lax.broadcasted_iota(jnp.int32, (TILE, HW), 1) < HW // 2

    def head_copy(tile):
        return remote(
            hsend.at[tile],
            heads.at[:, my_columns],
            hs.at[tile],
            hr.at[my_head],
            base + tile // 2,
            tile % 2,
        )

    def attend(tile):
        at = pl.multiple_of(tile * TILE, TILE)
        query = q_ref[pl.ds(at, TILE), :] * jnp.bfloat16(0.125)
        keys = k_ref[pl.ds(at, WINDOW * TILE), :]
        values = v_ref[pl.ds(at, WINDOW * TILE), :]
        zero = jnp.zeros_like(query)
        own = column(id_ref[2 * REACH + tile][0:1, :])
        same = [
            own == id_ref[tile + c][0:1, :].astype(jnp.float32) for c in range(WINDOW)
        ]
        lifted = []
        for part_query in (jnp.where(low, query, zero), jnp.where(low, zero, query)):
            scores = lax.dot_general(
                part_query, keys, (((1,), (1,)), ((), ())), preferred_element_type=jnp.float32
            )
            pieces = [
                jnp.where(same[c], scores[:, c * TILE : (c + 1) * TILE], -1e30)
                for c in range(WINDOW)
            ]
            peak = functools.reduce(jnp.maximum, pieces)
            peak = jnp.max(peak, axis=1, keepdims=True)
            pieces = [jnp.exp(piece - peak) for piece in pieces]
            total = jnp.sum(functools.reduce(jnp.add, pieces), axis=1, keepdims=True)
            lifted.append((pieces, total))
        (one, total1), (two, total2) = lifted
        scale1, scale2 = 1.0 / total1, lam / total2
        weights = jnp.concatenate(
            [
                (one[c] * scale1 - two[c] * scale2).astype(jnp.bfloat16)
                for c in range(WINDOW)
            ],
            axis=1,
        )
        out = jnp.dot(weights, values, preferred_element_type=jnp.float32)
        out = out * lax.rsqrt(jnp.mean(out * out, axis=1, keepdims=True) + 1e-6)
        return out.astype(jnp.bfloat16)

    def attend_step(j, _):
        tile = (mine + 1 + j) % 8
        hsend[tile] = attend(tile)

        @pl.when(j == EARLY - 1)
        def _():
            pl.semaphore_wait(barrier, CHIPS - 1 + GROUP)
            for n in range(EARLY - 1):
                head_copy((mine + 1 + n) % 8).start()

        @pl.when((j >= EARLY - 1) & (j < 7))
        def _():
            head_copy(tile).start()

        return 0

    lax.fori_loop(0, 8, attend_step, 0)
    heads[:, my_columns] = hsend[mine]
    loads[0].wait()
    lane = lax.broadcasted_iota(jnp.int32, (TILE, CHIPS * CAP), 1)
    mix = lax.rem((lane // CAP) * STRIDE, CHIPS)
    expert = (
        lax.rem(mz + lax.div(mix, 16), 4) * 16
        + lax.rem(my + lax.div(mix, 4), 4) * 4
        + lax.rem(mx + mix, 4)
    ).astype(jnp.float32)
    rank = (lane % CAP).astype(jnp.float32)

    first = wide(route_ref[0:1, :]) == expert
    second = wide(route_ref[1:2, :]) == expert
    named = jnp.where(first | second, 1.0, 0.0).astype(jnp.bfloat16)
    before = jnp.where(
        lax.broadcasted_iota(jnp.int32, (TILE, TILE), 0)
        > lax.broadcasted_iota(jnp.int32, (TILE, TILE), 1),
        1.0,
        0.0,
    ).astype(jnp.bfloat16)
    earlier = jnp.dot(before, named, preferred_element_type=jnp.float32)
    hit = jnp.where(earlier == rank, 1.0, 0.0)
    pick0 = jnp.where(first, hit, 0.0)
    pick1 = jnp.where(second, hit, 0.0)
    pick[0:TILE] = pick0.astype(jnp.bfloat16)
    pick[TILE:] = pick1.astype(jnp.bfloat16)
    pack = jnp.transpose(pick0 + pick1).astype(jnp.bfloat16)
    for load in loads[1:5]:
        load.wait()

    def head_wait(j, _):
        h = (my_head + 1 + j) % 8
        remote(
            hsend.at[0],
            heads.at[:, pl.ds(pl.multiple_of(h * HW, HW), HW)],
            hs.at[0],
            hr.at[h],
            me,
            other,
        ).wait_recv()
        return 0

    lax.fori_loop(0, 7, head_wait, 0)

    square = jnp.zeros((TILE, 1), jnp.float32)
    WIDE = 512
    for n in range(D // WIDE):
        cut = slice(n * WIDE, (n + 1) * WIDE)
        projected = jnp.dot(heads[...], wout[:, cut], preferred_element_type=jnp.float32)
        value = (res_ref[:, cut].astype(jnp.float32) + projected).astype(jnp.bfloat16)
        mixed[:, cut] = value
        value = value.astype(jnp.float32)
        square = square + jnp.sum(value * value, axis=1, keepdims=True)
    inverse = lax.rsqrt(square / D + 1e-6)
    for n in range(D // WIDE):
        cut = slice(n * WIDE, (n + 1) * WIDE)
        normed[:, cut] = (
            mixed[:, cut].astype(jnp.float32) * inverse * gain_ref[:, cut]
        ).astype(jnp.bfloat16)

    def block(i):
        return pl.ds(pl.multiple_of(i * CAP, CAP), CAP)

    def dispatch_copy(i):
        to = place(i, 1)
        return remote(
            outgoing.at[block(i)], rows.at[core, block(i)], ds_.at[i], dr.at[i], to, core
        )

    def return_copy(i):
        to = place(i, -1)
        return remote(answer.at[block(i)], returned.at[block(i)], rs.at[i], rr.at[i], to, core)

    def chunk(k):
        return pl.ds(k * ROWS, ROWS)

    def forward_copy(k):
        return remote(
            rows.at[core, chunk(k)], rows.at[core, chunk(k)], fs.at[k], fr.at[k], me, other
        )

    def part_copy(k):
        return remote(part.at[other, chunk(k)], theirs.at[chunk(k)], ps.at[k], pr.at[k], me, other)

    def each(start, stop, action):
        def body(i, _):
            action(i)
            return 0

        lax.fori_loop(start, stop, body, 0)

    for first_slot, last_slot in ((0, FIRST), (FIRST, CHIPS)):
        low_row, high_row = first_slot * CAP, last_slot * CAP
        for n in range(D // WIDE):
            cut = slice(n * WIDE, (n + 1) * WIDE)
            outgoing[low_row:high_row, cut] = jnp.dot(
                pack[low_row:high_row], normed[:, cut], preferred_element_type=jnp.float32
            ).astype(jnp.bfloat16)
        each(max(1, first_slot), last_slot, lambda i: dispatch_copy(i).start())
    rows[core, 0:CAP] = outgoing[0:CAP]
    for load in loads[5:]:
        load.wait()

    def compute(k):
        both = jnp.concatenate([rows[0, chunk(k)], rows[1, chunk(k)]], axis=0)
        NW = 256
        for n in range(FF // NW):
            cut = slice(n * NW, (n + 1) * NW)
            g = jnp.dot(both, gate[:, cut], preferred_element_type=jnp.float32)
            u = jnp.dot(both, upw[:, cut], preferred_element_type=jnp.float32)
            hidden[:, cut] = (g / (1.0 + jnp.exp(-g)) * u).astype(jnp.bfloat16)
        for n in range(D // 512):
            cut = slice(n * 512, (n + 1) * 512)
            o = jnp.dot(hidden[...], down[:, cut], preferred_element_type=jnp.float32)
            o = o.astype(jnp.bfloat16)
            part[0, chunk(k), cut] = o[:ROWS]
            part[1, chunk(k), cut] = o[ROWS:]

    def finish(k):
        part_copy(k).wait_recv()
        answer[chunk(k)] = (
            part[core, chunk(k)].astype(jnp.float32) + theirs[chunk(k)].astype(jnp.float32)
        ).astype(jnp.bfloat16)
        gone = 0 if k == 0 else GATE[k - 1]
        each(max(1, gone * PER), GATE[k] * PER, lambda i: dispatch_copy(i).wait_send())
        each(max(1, k * PER), (k + 1) * PER, lambda i: return_copy(i).start())
        if k == 0:
            returned[0:CAP] = answer[0:CAP]

    for k in range(CHUNKS):
        each(max(1, k * PER), (k + 1) * PER, lambda i: dispatch_copy(i).wait_recv())
        forward_copy(k).start()
        if k >= 1:
            finish(k - 1)
        forward_copy(k).wait_recv()
        compute(k)
        part_copy(k).start()
    finish(CHUNKS - 1)

    weight0, weight1 = wide(rw_ref[0:1, :]), wide(rw_ref[1:2, :])

    def weighted(low_row, high_row, cut):
        both = jnp.dot(
            pick[:, low_row:high_row],
            returned[low_row:high_row, cut],
            preferred_element_type=jnp.float32,
        )
        return both[:TILE] * weight0 + both[TILE:] * weight1

    each(1, TAIL, lambda i: return_copy(i).wait_recv())
    for n in range(D // WIDE):
        cut = slice(n * WIDE, (n + 1) * WIDE)
        sums[:, cut] = mixed[:, cut].astype(jnp.float32) + weighted(0, TAIL * CAP, cut)

    def head_sent(j, _):
        head_copy((mine + 1 + j) % 8).wait_send()
        return 0

    lax.fori_loop(0, 7, head_sent, 0)
    each(max(1, GATE[-1] * PER), CHIPS, lambda i: dispatch_copy(i).wait_send())
    each(1, CHIPS, lambda i: return_copy(i).wait_send())
    for k in range(CHUNKS):
        forward_copy(k).wait_send()
        part_copy(k).wait_send()
    each(TAIL, CHIPS, lambda i: return_copy(i).wait_recv())
    for n in range(D // WIDE):
        cut = slice(n * WIDE, (n + 1) * WIDE)
        out_ref[:, cut] = (sums[:, cut] + weighted(TAIL * CAP, CHIPS * CAP, cut)).astype(
            jnp.bfloat16
        )


def on_device(
    residual,
    query_rows,
    key_rows,
    value_rows,
    mix_lambda,
    documents,
    out_weight,
    norm_gain,
    gate_weight,
    up_weight,
    down_weight,
    routes,
    route_weights,
):
    q, k, v, ids, lam = gathered(query_rows, key_rows, value_rows, documents, mix_lambda)
    dma = pltpu.SemaphoreType.DMA
    bf = jnp.bfloat16
    total = CHIPS * CAP
    return pl.pallas_call(
        main_kernel,
        out_shape=pltpu.VMEM((TILE, D), bf),
        in_specs=[VMEM] * 5 + [ANY] * 8,
        out_specs=VMEM,
        scratch_shapes=[
            pltpu.VMEM((2, TILE), jnp.int32),
            pltpu.VMEM((TILE, D), bf),
            pltpu.VMEM((1, D), jnp.float32),
            pltpu.VMEM((2, TILE), jnp.float32),
            pltpu.VMEM((8 * HW, D), bf),
            pltpu.VMEM((D, FF), bf),
            pltpu.VMEM((D, FF), bf),
            pltpu.VMEM((FF, D), bf),
            pltpu.VMEM((8, TILE, HW), bf),
            pltpu.VMEM((TILE, 8 * HW), bf),
            pltpu.VMEM((TILE, D), bf),
            pltpu.VMEM((total, D), bf),
            pltpu.VMEM((2, total, D), bf),
            pltpu.VMEM((2 * ROWS, FF), bf),
            pltpu.VMEM((2, total, D), bf),
            pltpu.VMEM((total, D), bf),
            pltpu.VMEM((total, D), bf),
            pltpu.VMEM((total, D), bf),
            pltpu.VMEM((2 * TILE, total), bf),
            pltpu.VMEM((TILE, D), bf),
            pltpu.VMEM((TILE, D), jnp.float32),
            dma((8,)),
            dma((8,)),
            dma((8,)),
            dma((CHIPS,)),
            dma((CHIPS,)),
            dma((CHUNKS,)),
            dma((CHUNKS,)),
            dma((CHUNKS,)),
            dma((CHUNKS,)),
            dma((CHIPS,)),
            dma((CHIPS,)),
        ],
        compiler_params=pltpu.CompilerParams(
            collective_id=1, has_side_effects=True, vmem_limit_bytes=46 * 1024 * 1024
        ),
    )(
        *(
            pltpu.with_memory_space_constraint(a, pltpu.VMEM)
            for a in (
                q.reshape(GROUP * LEN, HW),
                k.reshape(SLOTS * LEN, HW),
                v.reshape(SLOTS * LEN, HW),
                ids.reshape(2 * SLOTS, 8, TILE),
                lam,
            )
        ),
        *(
            pltpu.with_memory_space_constraint(a, pltpu.HBM)
            for a in (
                routes.T,
                residual,
                norm_gain.reshape(1, D),
                route_weights.T,
                out_weight,
                gate_weight,
                up_weight,
                down_weight,
            )
        ),
    )


def solution(mesh):
    placed = (
        P(("sp", "tp"), None),
        P("sp", "tp"),
        P("sp", "tp"),
        P("sp", "tp"),
        P("tp"),
        P("sp"),
        P(),
        P(),
        P("sp", None, "tp"),
        P("sp", None, "tp"),
        P("sp", "tp", None),
        P(("sp", "tp"), None),
        P(("sp", "tp"), None),
    )
    return jax.shard_map(
        on_device, mesh=mesh, in_specs=placed, out_specs=P(("sp", "tp"), None), check_vma=False
    )
```
